32 devices in a mesh: ep: 8 (over z, x), tp: 4 (over y, core).
Axes of the slice: x: 2, y: 2, z: 4, core: 2. Of those that a mesh axis runs over, the one named last changes fastest.
Arguments:
- mix_bgate: bfloat16 [2048, 1024], P('ep', 'tp'), may hold values from -6 to 6
- mix_cgate: bfloat16 [2048, 1024], P('ep', 'tp'), may hold values from -6 to 6
- mix_input: bfloat16 [2048, 1024], P('ep', 'tp'), may hold values from -6 to 6
- conv_taps: float32 [3, 1024], P(None, 'tp'), may hold values from -3.5 to 3.5
- mix_out_w: bfloat16 [1024, 2048], P('tp'), may hold values from -0.1875 to 0.1875
- moe_x: bfloat16 [2048, 2048], P('ep', 'tp'), may hold values from -6 to 6
- moe_gain: float32 [2048], replicated, may hold values from 0.1 to 1.9
- routes: int32 [2048, 2], P('ep'), may hold values from 0 to 7, all different within a row; in each aligned block of 256 rows (0 to 255, 256 to 511, ...) at most 96 rows name the same one
- route_w: float32 [2048, 2], P('ep'), may hold values from 0.2 to 1
- w_gate: bfloat16 [8, 2048, 3584], P('ep', None, 'tp'), may hold values from -0.125 to 0.125
- w_up: bfloat16 [8, 2048, 3584], P('ep', None, 'tp'), may hold values from -0.125 to 0.125
- w_down: bfloat16 [8, 3584, 2048], P('ep', 'tp'), may hold values from -0.09375 to 0.09375
Outputs:
- mixed: bfloat16 [2048, 2048], P(('ep', 'tp'))
- routed: bfloat16 [2048, 2048], P('ep', 'tp')
The draws below stay inside these ranges and needn't reach their ends.
Inputs may be any that keep to these rules, and one draw needn't show every extreme that they name: `routes`: among the 256 rows of one index of ep, each row names 2 different experts and no expert is named by more than 96 rows; in every draw some expert is named by exactly 96 rows of some index.
All inputs are finite; a program needn't handle non-finite values.
Results may differ from the reference program's by a relative error of at most 0.012.
Values may be sent and summed in bfloat16 or wider, within the bound.
A program may use at most 64 MiB of HBM per device.

```python
import math
import jax
import jax.numpy as jnp
import numpy as np
from jax import lax

D = 2048
CONV = 1024
TAPS = 3
FF_E = 3584
TOPK = 2
TOK_MOE = 256
SEQ = 2048
MOE_TOKENS = 2048
EXPERTS = 8
CAP = 96
N_EP = 8
N_TP = 4


def steps_of(stream_key, shape, split, low, top_value):
    def one(position, shards_of):
        steps = jax.random.uniform(jax.random.fold_in(jax.random.fold_in(stream_key, 6), position), (shards_of,), jnp.float32, low / len(split), top_value / len(split))
        return jnp.repeat(jnp.exp(steps), shape[position] // shards_of).reshape((-1,) + (1,) * (len(shape) - position - 1))

    loudness = one(*split[0])
    for cut in split[1:]:
        loudness = loudness * one(*cut)
    return loudness


def assign_block(own_key, own, number, rows, amount, top, bound, skew):
    sequence = jax.random.permutation(own_key, amount)
    heavy_load, ordinary = portions_of(amount, rows * top, bound, skew, True), portions_of(amount, rows * top, bound, skew, False)
    places = jnp.arange(amount)

    def named(lengths, offset_by):
        used = int((lengths > 0).sum())
        fixed = max(1, used // 4)
        moved = fixed + (places - fixed + offset_by * (used - fixed)) % max(1, amount - fixed)
        return jnp.zeros((amount,), jnp.int32).at[sequence[jnp.where(places < fixed, places, moved)]].set(jnp.asarray(lengths, jnp.int32))

    lengths = jnp.where(number % 4 == 0, named(heavy_load, number // 4), named(ordinary, number - number // 4 - 1))
    mixed = jax.random.permutation(jax.random.fold_in(own, 3), amount)
    source_of, taker = mixed[0:amount // 2 * 2:2], mixed[1:amount // 2 * 2:2]
    slack = jnp.minimum(lengths[source_of] - 1, bound - lengths[taker]) // 2
    slack = jnp.where((source_of == sequence[0]) | (taker == sequence[0]) | (lengths[taker] == 0), 0, jnp.maximum(slack, 0))
    moved = jax.random.randint(jax.random.fold_in(own, 4), (amount // 2,), 0, 1 << 20) % (slack + 1)
    lengths = lengths.at[source_of].add(-moved).at[taker].add(moved)
    items = jnp.searchsorted(jnp.cumsum(lengths), jnp.arange(rows * top), side="right").astype(jnp.int32)
    listing = items.reshape(top, rows).T
    listing = listing[jax.random.permutation(jax.random.fold_in(own, 1), rows)]
    offset_by = jax.random.randint(jax.random.fold_in(own, 2), (rows, 1), 0, top)
    return jnp.take_along_axis(listing, (jnp.arange(top)[None, :] + offset_by) % top, axis=1)


def portions_of(amount, total, reach, lean, full):
    loads = [(1 << 20) // math.isqrt(grade ** lean) + 1 for grade in range(1, amount + 1)]
    largest = reach if full else min(reach, max(-(-total // amount), total * loads[0] // sum(loads)))
    least = 1 if total - largest >= amount - 1 else 0
    counts, surplus = [largest] + [least] * (amount - 1), total - largest - least * (amount - 1)
    while surplus > 0:
        candidates = [i for i in range(1, amount) if counts[i] < largest] or [i for i in range(1, amount) if counts[i] < reach]
        pool, budget = sum([loads[i] for i in candidates]), surplus
        for i in candidates:
            more = min(reach - counts[i], max(1, budget * loads[i] // pool), surplus)
            counts[i] = counts[i] + more
            surplus = surplus - more
    return np.array(counts)


def normal_values(rng, extent, spread, reach, shards=(), kind=jnp.bfloat16):
    factor_of = steps_of(rng, extent, shards, -0.22, 0.18) if shards else 1.0
    array = jax.random.normal(rng, extent, jnp.float32) * spread * factor_of
    return jnp.minimum(jnp.maximum(array, -reach), reach).astype(kind)


def setup_inputs(seed: int = 0) -> dict:
    key_of = jax.random.split(jax.random.key(seed), 13)
    mix_bgate = normal_values(key_of[0], (SEQ, CONV), 1.0, 6.0, ((0, 8), (1, 4)))
    mix_cgate = normal_values(key_of[1], (SEQ, CONV), 1.0, 6.0, ((0, 8), (1, 4)))
    mix_input = normal_values(key_of[2], (SEQ, CONV), 1.0, 6.0, ((0, 8), (1, 4)))
    conv_taps = normal_values(key_of[3], (TAPS, CONV), TAPS ** -0.5, 3.5, ((1, 4),), jnp.float32)
    mix_out_w = normal_values(key_of[4], (CONV, D), CONV ** -0.5, 0.1875, ((0, 4),))
    moe_x = normal_values(key_of[5], (MOE_TOKENS, D), 1.0, 6.0, ((0, 8), (1, 4)))
    moe_gain = jnp.clip(1.0 + 0.18 * jax.random.normal(key_of[6], (D,), jnp.float32), 0.1, 1.9)
    routes_keys = jax.random.split(jax.random.fold_in(key_of[7], 1), MOE_TOKENS // TOK_MOE)
    routes_turns = jax.random.permutation(jax.random.fold_in(key_of[7], 3), MOE_TOKENS // TOK_MOE)
    routes = jax.vmap(lambda own, number: assign_block(jax.random.fold_in(key_of[7], 2), own, number, TOK_MOE, EXPERTS, TOPK, CAP, 2))(routes_keys, routes_turns).reshape((MOE_TOKENS, TOPK))
    route_w = jnp.clip(0.2 + 0.8 * jax.random.uniform(key_of[8], (MOE_TOKENS, TOPK), jnp.float32) ** steps_of(key_of[8], (MOE_TOKENS, TOPK), ((0, 8),), -0.2, 0.2), 0.2, 1.0)
    w_gate = normal_values(key_of[9], (EXPERTS, D, FF_E), D ** -0.5, 0.125, ((0, 8), (2, 4)))
    w_up = normal_values(key_of[10], (EXPERTS, D, FF_E), D ** -0.5, 0.125, ((0, 8), (2, 4)))
    w_down = normal_values(key_of[11], (EXPERTS, FF_E, D), FF_E ** -0.5, 0.09375, ((0, 8), (1, 4)))
    return {"mix_bgate": mix_bgate, "mix_cgate": mix_cgate, "mix_input": mix_input, "conv_taps": conv_taps, "mix_out_w": mix_out_w, "moe_x": moe_x, "moe_gain": moe_gain, "routes": routes, "route_w": route_w, "w_gate": w_gate, "w_up": w_up, "w_down": w_down}


def rms_rows(values, gain):
    wide = values.astype(jnp.float32)
    scale = lax.rsqrt(lax.optimization_barrier(jnp.mean(wide * wide, axis=-1, keepdims=True)) + 1e-06)
    return (wide * scale * gain).astype(jnp.bfloat16)

def rounded(value):
    return lax.optimization_barrier(value.astype(jnp.bfloat16)).astype(jnp.float32)

def reference(mix_bgate, mix_cgate, mix_input, conv_taps, mix_out_w, moe_x, moe_gain, routes, route_w, w_gate, w_up, w_down):
    length = mix_input.shape[0]
    prod = mix_cgate.astype(jnp.float32) * mix_input.astype(jnp.float32)
    padded = jnp.pad(prod, ((TAPS - 1, 0), (0, 0)))
    conv = conv_taps[0] * padded[0:length]
    for j in range(1, TAPS):
        conv = conv + conv_taps[j] * padded[j:j + length]
    gated = (mix_bgate.astype(jnp.float32) * conv).astype(jnp.bfloat16)
    step = CONV // N_TP
    total = jnp.zeros((length, D), jnp.float32)
    for q in range(N_TP):
        part = jnp.dot(gated[:, q * step:(q + 1) * step], mix_out_w[q * step:(q + 1) * step], preferred_element_type=jnp.float32)
        total = total + rounded(part)
    mixed = total.astype(jnp.bfloat16)
    normed = rms_rows(moe_x, moe_gain)
    dev_routes = routes.reshape(N_EP, TOK_MOE * TOPK)
    onehot = (dev_routes[:, :, None] == jnp.arange(EXPERTS, dtype=jnp.int32)[None, None, :]).astype(jnp.int32)
    earlier = jnp.cumsum(onehot, axis=1) - onehot
    slot = lax.optimization_barrier(jnp.sum(earlier * onehot, axis=2))
    row = jnp.arange(N_EP, dtype=jnp.int32)[:, None] * CAP + slot
    flat_e = dev_routes.reshape(-1)
    flat_row = row.reshape(-1).astype(jnp.int32)
    token = jnp.arange(MOE_TOKENS * TOPK, dtype=jnp.int32) // TOPK
    buffers = jnp.zeros((EXPERTS, N_EP * CAP, D), jnp.bfloat16).at[flat_e, flat_row].set(normed[token])
    fstep = FF_E // N_TP

    def expert(items):
        rows, wg, wu, wd = items
        gate = jnp.dot(rows, wg, preferred_element_type=jnp.float32)
        upper = jnp.dot(rows, wu, preferred_element_type=jnp.float32)
        hidden = (jax.nn.silu(gate) * upper).astype(jnp.bfloat16)
        acc = jnp.zeros((rows.shape[0], D), jnp.float32)
        for q in range(N_TP):
            part = jnp.dot(hidden[:, q * fstep:(q + 1) * fstep], wd[q * fstep:(q + 1) * fstep], preferred_element_type=jnp.float32)
            acc = acc + rounded(part)
        return acc.astype(jnp.bfloat16)
    results = lax.map(expert, (buffers, w_gate, w_up, w_down))
    picked = results[flat_e, flat_row].astype(jnp.float32).reshape(MOE_TOKENS, TOPK, D)
    routed = lax.optimization_barrier(jnp.sum(picked * route_w[:, :, None], axis=1)).astype(jnp.bfloat16)
    return (mixed, routed)
```

```python
import functools

import jax
import jax.numpy as jnp
from jax import lax
from jax.experimental import pallas as pl
from jax.experimental.pallas import tpu as pltpu
from jax.sharding import PartitionSpec as P

BF16 = jnp.bfloat16
F32 = jnp.float32
MESH = pl.DeviceIdType.MESH


def flip(index, bits):
    bit = 1
    while bit <= bits:
        if bits & bit:
            index = index + bit - 2 * bit * ((index // bit) % 2)
        bit *= 2
    return index


def split_terms(value):
    high = value.astype(BF16)
    return high, (value - high.astype(F32)).astype(BF16)


def dot(a, b):
    return jnp.dot(a, b, preferred_element_type=F32)


def sizes_of(ntok, top, experts):
    cap = 4 * ((3 * ntok * top + 8 * experts - 1) // (8 * experts))
    return -(-cap // 16) * 16


def kernel(
    n_ep,
    n_tp,
    cap,
    per_group,
    bgate,
    cgate,
    inputs,
    taps,
    out_w,
    x,
    gain,
    routes,
    routes_t,
    route_w,
    w_gate,
    w_up,
    w_down,
    mixed,
    routed,
    wgu,
    wd,
    wo,
    halo,
    prod,
    gated,
    share,
    share_in,
    share_sum,
    share_far,
    squares,
    sent,
    rows,
    hidden,
    part,
    part_in,
    part_sum,
    part_far,
    final,
    back,
    at_high,
    at_low,
    total,
    gate_sem,
    up_sem,
    plain_sem,
    halo_sem,
    square_sem,
    share_sem,
    go_sem,
    far_sem,
    near_sem,
    near2_sem,
    part_sem,
    part_far_sem,
    back_sem,
):
    ep = lax.axis_index("ep")
    tp = lax.axis_index("tp")
    ntok, d = x.shape
    length, chans = cgate.shape
    reach = taps.shape[0] - 1
    d_all = n_tp * d
    ff = w_down.shape[1]
    groups = n_ep // per_group
    grows = per_group * cap
    near = flip(tp, 1)
    far = flip(tp, 2)
    cross = flip(tp, 3)
    mine = pl.ds(pl.multiple_of(tp * d, 128), d)
    theirs = pl.ds(pl.multiple_of(far * d, 128), d)
    next_ep = (ep + 1) % n_ep

    tiles = ff // 128
    loads = []
    for i in range(tiles):
        for src, sem, at in ((w_gate, gate_sem, 0), (w_up, up_sem, 128)):
            copy = pltpu.make_async_copy(
                src.at[0, :, pl.ds(i * 128, 128)], wgu.at[:, pl.ds(i * 256 + at, 128)], sem.at[i]
            )
            copy.start()
            loads.append(copy)
    down_load = pltpu.make_async_copy(w_down.at[0], wd, plain_sem.at[0])
    down_load.start()
    loads.append(down_load)
    out_load = pltpu.make_async_copy(out_w, wo, plain_sem.at[1])
    out_load.start()

    barrier = pltpu.get_barrier_semaphore()
    for j in range(1, n_ep):
        pl.semaphore_signal(barrier, inc=1, device_id=(flip(ep, j), tp), device_id_type=MESH)
    for t in (near, far, cross):
        pl.semaphore_signal(barrier, inc=1, device_id=(ep, t), device_id_type=MESH)

    def slots_by_lane():
        e_iota = lax.broadcasted_iota(jnp.int32, (n_ep, ntok), 0)
        chosen = [routes_t[k : k + 1, :] == e_iota for k in range(2)]
        named = jnp.where(chosen[0] | chosen[1], 1.0, 0.0).astype(BF16)
        row = lax.broadcasted_iota(jnp.int32, (ntok, ntok), 0)
        col = lax.broadcasted_iota(jnp.int32, (ntok, ntok), 1)
        rank = dot(named, jnp.where(row < col, 1.0, 0.0).astype(BF16))
        slot = rank + (e_iota * cap).astype(F32)
        return [jnp.sum(jnp.where(c, slot, 0.0), axis=0, keepdims=True) for c in chosen]

    lane_slots = slots_by_lane()
    wide = x[...].astype(F32)
    ones = jnp.ones((8, d), BF16)
    own_squares = jnp.zeros((8, ntok), F32)
    for term in split_terms(wide * wide):
        own_squares = own_squares + lax.dot_general(
            ones, term, (((1,), (1,)), ((), ())), preferred_element_type=F32
        )
    squares[tp] = own_squares

    pl.semaphore_wait(barrier, n_ep + 2)

    def remote(src, dst, sems, i, device):
        return pltpu.make_async_remote_copy(
            src_ref=src,
            dst_ref=dst,
            send_sem=sems.at[0, i],
            recv_sem=sems.at[1, i],
            device_id=device,
            device_id_type=MESH,
        )

    started = []

    def send(copy):
        copy.start()
        started.append(copy)

    square_copies = [
        remote(squares.at[tp], squares.at[tp], square_sem, i, (ep, flip(tp, i + 1)))
        for i in range(3)
    ]
    for copy in square_copies:
        send(copy)
    halo_copies = [
        remote(ref.at[pl.ds(length - 16, 16)], halo.at[i], halo_sem, i, (next_ep, tp))
        for i, ref in enumerate((cgate, inputs))
    ]
    for copy in halo_copies:
        send(copy)

    for copy in square_copies:
        copy.wait_recv()
    sums = squares[0]
    for i in range(1, n_tp):
        sums = sums + squares[i]
    scale = lax.rsqrt(sums / d_all + 1e-06)[0:1, :]

    def block(i):
        return pl.ds(pl.multiple_of(i * cap, 16), cap)

    def group_rows(g):
        first = flip(ep, g * per_group) // per_group * per_group
        return first, pl.ds(pl.multiple_of(first * cap, 16), grows)

    go = [None] * n_ep
    own_gain = gain[:, mine]
    for g in range(groups):
        first, span = group_rows(g)
        at = (lax.broadcasted_iota(jnp.int32, (grows, ntok), 0) + first * cap).astype(F32)
        hit = (at == lane_slots[0]) | (at == lane_slots[1])
        high, low = split_terms(jnp.where(hit, scale, 0.0))
        picked = (dot(high, x[...]) + dot(low, x[...])) * own_gain
        sent[span] = picked.astype(BF16)
        for j in range(g * per_group, (g + 1) * per_group):
            if j == 0:
                rows[block(ep), mine] = sent[block(ep)]
            else:
                to = flip(ep, j)
                go[j] = remote(sent.at[block(to)], rows.at[block(ep), mine], go_sem, j, (to, tp))
                send(go[j])

    def hop(j, columns, sems, device):
        at = (block(flip(ep, j)), columns)
        return remote(rows.at[at], rows.at[at], sems, j, (ep, device))

    to_far = [hop(j, mine, far_sem, far) for j in range(n_ep)]
    to_near = [hop(j, mine, near_sem, near) for j in range(n_ep)]
    on_near = [hop(j, theirs, near2_sem, near) for j in range(n_ep)]

    def arrive(js):
        for j in js:
            if j:
                go[j].wait_recv()
            send(to_far[j])
            send(to_near[j])

    def relay(js):
        for j in js:
            to_far[j].wait_recv()
            send(on_near[j])

    def ready(js):
        for j in js:
            to_near[j].wait_recv()
            on_near[j].wait_recv()

    order = (cross, near, far, tp)

    part_copies = [[None, None] for _ in range(groups)]
    part_far_copies = [None] * groups
    back_copies = [None] * n_ep

    def compute(g):
        _, span = group_rows(g)

        def tile(i, carry):
            both = dot(rows[span, :], wgu[:, pl.ds(pl.multiple_of(i * 256, 256), 256)])
            gate, upper = both[:, :128], both[:, 128:]
            act = gate / (1.0 + jnp.exp(-gate)) * upper
            hidden[:, pl.ds(pl.multiple_of(i * 128, 128), 128)] = act.astype(BF16)
            return carry

        lax.fori_loop(0, tiles, tile, 0)
        for k, p in enumerate(order):
            columns = pl.ds(pl.multiple_of(p * d, 128), d)
            part[g, k] = dot(hidden[...], wd[:, columns]).astype(BF16)
            if k < 2:
                part_copies[g][k] = remote(
                    part.at[g, k], part_in.at[g, k], part_sem, 2 * g + k, (ep, near)
                )
                send(part_copies[g][k])

    def add_near(g):
        part_copies[g][0].wait_recv()
        part_sum[g] = (part[g, 2].astype(F32) + part_in[g, 0].astype(F32)).astype(BF16)
        part_far_copies[g] = remote(
            part_sum.at[g], part_far.at[g], part_far_sem, g, (ep, far)
        )
        send(part_far_copies[g])

    def add_far(g):
        first, span = group_rows(g)
        part_copies[g][1].wait_recv()
        near_sum = part[g, 3].astype(F32) + part_in[g, 1].astype(F32)
        part_far_copies[g].wait_recv()
        final[span] = (near_sum + part_far[g].astype(F32)).astype(BF16)
        for j in range(g * per_group, (g + 1) * per_group):
            if j == 0:
                back[block(ep)] = final[block(ep)]
            else:
                to = flip(ep, j)
                back_copies[j] = remote(
                    final.at[block(to)], back.at[block(ep)], back_sem, j, (to, tp)
                )
                send(back_copies[j])

    def collect(g):
        _, span = group_rows(g)
        for j in range(g * per_group, (g + 1) * per_group):
            if j:
                back_copies[j].wait_recv()
        got = back[span]
        now = dot(at_high[g], got) + dot(at_low[g], got)
        if g == 0:
            total[...] = now
        elif g < groups - 1:
            total[...] += now
        else:
            routed[...] = (total[...] + now).astype(BF16)

    part_rows = length // n_tp

    def part_of(p):
        return pl.ds(pl.multiple_of(p * part_rows, 16), part_rows)

    share_copies = []

    def mix():
        for copy in halo_copies:
            copy.wait_recv()
        before = halo[0].astype(F32) * halo[1].astype(F32)
        prod[0:16, :] = jnp.where(ep > 0, before, 0.0)
        prod[16:, :] = cgate[...].astype(F32) * inputs[...].astype(F32)
        conv = taps[0:1, :] * prod[16 - reach : 16 - reach + length, :]
        for j in range(1, reach + 1):
            conv = conv + taps[j : j + 1, :] * prod[16 - reach + j : 16 - reach + j + length, :]
        gated[...] = (bgate[...].astype(F32) * conv).astype(BF16)
        out_load.wait()

        def tile(i, carry):
            columns = pl.ds(pl.multiple_of(i * 256, 256), 256)
            share[:, columns] = dot(gated[...], wo[:, columns]).astype(BF16)
            return carry

        lax.fori_loop(0, d_all // 256, tile, 0)
        for k in range(2):
            share_copies.append(
                remote(share.at[part_of(order[k])], share_in.at[k], share_sem, k, (ep, near))
            )
            send(share_copies[k])

    def mix_near():
        share_copies[0].wait_recv()
        share_sum[...] = (
            share[part_of(far), :].astype(F32) + share_in[0].astype(F32)
        ).astype(BF16)
        share_copies.append(remote(share_sum, share_far, share_sem, 2, (ep, far)))
        send(share_copies[2])

    def mix_far():
        share_copies[1].wait_recv()
        near_sum = share[part_of(tp), :].astype(F32) + share_in[1].astype(F32)
        share_copies[2].wait_recv()
        mixed[...] = (near_sum + share_far[...].astype(F32)).astype(BF16)

    def tables():
        e_iota = lax.broadcasted_iota(jnp.int32, (ntok, n_ep), 1)
        chosen = [routes[:, k : k + 1] == e_iota for k in range(2)]
        named = jnp.where(chosen[0] | chosen[1], 1.0, 0.0).astype(BF16)
        row = lax.broadcasted_iota(jnp.int32, (ntok, ntok), 0)
        col = lax.broadcasted_iota(jnp.int32, (ntok, ntok), 1)
        rank = dot(jnp.where(col < row, 1.0, 0.0).astype(BF16), named)
        slot = rank + (e_iota * cap).astype(F32)
        slots = [jnp.sum(jnp.where(c, slot, 0.0), axis=1, keepdims=True) for c in chosen]
        for g in range(groups):
            first, _ = group_rows(g)
            at = (lax.broadcasted_iota(jnp.int32, (ntok, grows), 1) + first * cap).astype(F32)
            value = jnp.where(at == slots[0], route_w[:, 0:1], 0.0) + jnp.where(
                at == slots[1], route_w[:, 1:2], 0.0
            )
            at_high[g], at_low[g] = split_terms(value)

    half = per_group // 2

    def first_half(g):
        return range(g * per_group, g * per_group + half)

    def second_half(g):
        return range(g * per_group + half, (g + 1) * per_group)

    def whole(g):
        return range(g * per_group, (g + 1) * per_group)

    arrive(first_half(0))
    mix()
    arrive(second_half(0))
    mix_near()
    tables()
    arrive(whole(1))
    relay(whole(0))
    for load in loads:
        load.wait()
    for g in range(groups):
        if g + 2 < groups:
            arrive(first_half(g + 2))
        ready(whole(g))
        compute(g)
        if g + 1 < groups:
            relay(whole(g + 1))
        if g + 2 < groups:
            arrive(second_half(g + 2))
        add_near(g)
        if g:
            add_far(g - 1)
    add_far(groups - 1)
    mix_far()
    for g in range(groups):
        collect(g)
    for copy in started:
        copy.wait_send()


def body(
    mix_bgate,
    mix_cgate,
    mix_input,
    conv_taps,
    mix_out_w,
    moe_x,
    moe_gain,
    routes,
    route_w,
    w_gate,
    w_up,
    w_down,
):
    ntok, d = moe_x.shape
    length, chans = mix_input.shape
    n_ep = lax.axis_size("ep")
    n_tp = lax.axis_size("tp")
    assert w_gate.shape[0] == 1 and n_tp == 4 and routes.shape[1] == 2
    assert n_ep & (n_ep - 1) == 0
    cap = sizes_of(ntok, routes.shape[1], n_ep)
    per_group = 2
    while per_group * cap < 192 and 2 * per_group * 2 <= n_ep:
        per_group *= 2
    groups = n_ep // per_group
    grows = per_group * cap
    d_all = n_tp * d
    ff = w_down.shape[1]
    slots = n_ep * cap
    part_rows = length // n_tp
    vmem = pl.BlockSpec(memory_space=pltpu.VMEM)
    anywhere = pl.BlockSpec(memory_space=pl.ANY)
    dma = pltpu.SemaphoreType.DMA
    call = pl.pallas_call(
        functools.partial(kernel, n_ep, n_tp, cap, per_group),
        out_shape=(
            jax.ShapeDtypeStruct((part_rows, d_all), BF16),
            jax.ShapeDtypeStruct((ntok, d), BF16),
        ),
        in_specs=[vmem] * 4 + [anywhere] + [vmem] * 5 + [anywhere] * 3,
        out_specs=(vmem, vmem),
        scratch_shapes=[
            pltpu.VMEM((d_all, 2 * ff), BF16),
            pltpu.VMEM((ff, d_all), BF16),
            pltpu.VMEM((chans, d_all), BF16),
            pltpu.VMEM((2, 16, chans), BF16),
            pltpu.VMEM((16 + length, chans), F32),
            pltpu.VMEM((length, chans), BF16),
            pltpu.VMEM((length, d_all), BF16),
            pltpu.VMEM((2, part_rows, d_all), BF16),
            pltpu.VMEM((part_rows, d_all), BF16),
            pltpu.VMEM((part_rows, d_all), BF16),
            pltpu.VMEM((n_tp, 8, ntok), F32),
            pltpu.VMEM((slots, d), BF16),
            pltpu.VMEM((slots, d_all), BF16),
            pltpu.VMEM((grows, ff), BF16),
            pltpu.VMEM((groups, 4, grows, d), BF16),
            pltpu.VMEM((groups, 2, grows, d), BF16),
            pltpu.VMEM((groups, grows, d), BF16),
            pltpu.VMEM((groups, grows, d), BF16),
            pltpu.VMEM((slots, d), BF16),
            pltpu.VMEM((slots, d), BF16),
            pltpu.VMEM((groups, ntok, grows), BF16),
            pltpu.VMEM((groups, ntok, grows), BF16),
            pltpu.VMEM((ntok, d), F32),
            dma((ff // 128,)),
            dma((ff // 128,)),
            dma((2,)),
            dma((2, 2)),
            dma((2, 3)),
            dma((2, 3)),
            dma((2, n_ep)),
            dma((2, n_ep)),
            dma((2, n_ep)),
            dma((2, n_ep)),
            dma((2, 2 * groups)),
            dma((2, groups)),
            dma((2, n_ep)),
        ],
        compiler_params=pltpu.CompilerParams(
            collective_id=0, has_side_effects=True, vmem_limit_bytes=56 << 20
        ),
        name="step",
    )
    return call(
        mix_bgate,
        mix_cgate,
        mix_input,
        conv_taps,
        mix_out_w,
        moe_x,
        moe_gain.reshape(1, d_all),
        routes,
        routes.T,
        route_w,
        w_gate,
        w_up,
        w_down,
    )


def solution(mesh):
    in_specs = (
        P("ep", "tp"),
        P("ep", "tp"),
        P("ep", "tp"),
        P(None, "tp"),
        P("tp", None),
        P("ep", "tp"),
        P(),
        P("ep", None),
        P("ep", None),
        P("ep", None, "tp"),
        P("ep", None, "tp"),
        P("ep", "tp", None),
    )
    out_specs = (P(("ep", "tp"), None), P("ep", "tp"))
    return jax.shard_map(body, mesh=mesh, in_specs=in_specs, out_specs=out_specs, check_vma=False)
```

```python
import functools

import jax
import jax.numpy as jnp
from jax import lax
from jax.experimental import pallas as pl
from jax.experimental.pallas import tpu as pltpu
from jax.sharding import PartitionSpec as P

BF16 = jnp.bfloat16
F32 = jnp.float32
MESH = pl.DeviceIdType.MESH
scope = jax.named_scope

PLAN = (
    "D4", "D6", "D1", "D2", "D3", "A0", "S", "X", "T", "A1", "Q", "A4", "P", "G2", "G1", "D5",
    "G3", "D7", "B0", "Y0", "A2", "R4", "A6", "Y1", "L", "C4", "A3", "B2", "O4", "R6", "C0",
    "N4", "A5", "O0", "Y2", "B1", "B3", "C6", "F4", "O6", "A7", "N0", "N6", "C1", "R5", "O1",
    "Y3", "N1", "C5", "F6", "R7", "O5", "H0", "N5", "C7", "H1", "O7", "M0", "N7", "F5", "M1",
    "W", "F7", "Z", "K4", "K0", "K6", "K1", "K5", "K7", "E",
)


def flip(index, bits):
    bit = 1
    while bit <= bits:
        if bits & bit:
            index = index + bit - 2 * bit * ((index // bit) % 2)
        bit *= 2
    return index


def split_terms(value):
    high = value.astype(BF16)
    return high, (value - high.astype(F32)).astype(BF16)


def dot(a, b):
    return jnp.dot(a, b, preferred_element_type=F32)


def sizes_of(ntok, top, experts):
    cap = 4 * ((3 * ntok * top + 8 * experts - 1) // (8 * experts))
    return -(-cap // 16) * 16


def kernel(
    n_ep,
    n_tp,
    cap,
    bgate_in,
    cgate_in,
    inputs_in,
    taps_in,
    out_w,
    x_in,
    gain_in,
    routes_in,
    weight_in,
    w_gate,
    w_up,
    w_down,
    mixed,
    routed,
    x,
    routes_t,
    inputs,
    cgate,
    bgate,
    taps,
    weight_t,
    gain,
    wgu,
    wd,
    wo,
    halo,
    prod,
    gated,
    share,
    share_in,
    share_sum,
    share_far,
    x_far,
    sent,
    sent_far,
    rows,
    normed,
    hidden,
    part,
    part_in,
    part_sum,
    part_far,
    final,
    back,
    back_far,
    at_high,
    at_low,
    total,
    total_far,
    total_out,
    total_in,
    in_sem,
    gate_sem,
    up_sem,
    plain_sem,
    halo_sem,
    share_sem,
    cross_sem,
    go_sem,
    go_far_sem,
    far_sem,
    near_sem,
    near2_sem,
    part_sem,
    part_far_sem,
    back_sem,
    back_far_sem,
):
    ep = lax.axis_index("ep")
    tp = lax.axis_index("tp")
    ntok, d = x_in.shape
    length, chans = cgate_in.shape
    reach = taps_in.shape[0] - 1
    d_all = n_tp * d
    ff = w_down.shape[1]
    run_length = n_ep // 8
    near = flip(tp, 1)
    far = flip(tp, 2)
    cross = flip(tp, 3)
    mine = pl.ds(pl.multiple_of(tp * d, 128), d)
    theirs = pl.ds(pl.multiple_of(far * d, 128), d)
    next_ep = (ep + 1) % n_ep

    barrier = pltpu.get_barrier_semaphore()
    for j in range(1, n_ep):
        pl.semaphore_signal(barrier, inc=1, device_id=(flip(ep, j), tp), device_id_type=MESH)
    for t in (near, far):
        pl.semaphore_signal(barrier, inc=1, device_id=(ep, t), device_id_type=MESH)

    def load(i, source, dest):
        copy = pltpu.make_async_copy(source, dest, in_sem.at[i])
        copy.start()
        return copy

    first_loads = [load(0, routes_in, routes_t), load(1, x_in, x)]
    mix_loads = [
        load(2, inputs_in, inputs),
        load(3, cgate_in, cgate),
        load(4, bgate_in, bgate),
        load(5, taps_in, taps),
        load(6, out_w, wo),
    ]
    late_loads = [load(7, weight_in, weight_t), load(8, gain_in, gain)]

    def wait_all(copies):
        for copy in copies:
            copy.wait()
        copies.clear()

    def run_of(r):
        return range(r * run_length, (r + 1) * run_length)

    def place(i):
        low, run, high = i % run_length, i // run_length % 4, i // run_length // 4
        return (4 * high + 2 * (run % 2) + run // 2) * run_length + low

    def block(i):
        return pl.ds(pl.multiple_of(place(i) * cap, 16), cap)

    half = ep // (4 * run_length) % 2
    step = ep // (2 * run_length) % 2
    inner = half + step - 2 * half * step

    def member(j):
        to = flip(ep, j)
        if j < 4 * run_length:
            return to
        wanted = half if j // (2 * run_length) % 2 else 1 - half
        return to + 2 * run_length * (wanted - to // (2 * run_length) % 2)

    def seen_as(j):
        if j < 4 * run_length:
            return j
        run, low = j // run_length, j % run_length
        return (4 + 2 * inner + run % 2) * run_length + low

    def rows_of(unit):
        count = len(unit) * run_length
        first = place(member(unit[0] * run_length)) // count * count * cap
        return first, count * cap

    def span_of(unit):
        first, count = rows_of(unit)
        return pl.ds(pl.multiple_of(first, 16), count)

    def slots_by_lane():
        e_iota = lax.broadcasted_iota(jnp.int32, (n_ep, ntok), 0)
        chosen = [routes_t[k : k + 1, :] == e_iota for k in range(2)]
        named = jnp.where(chosen[0] | chosen[1], 1.0, 0.0).astype(BF16)
        row = lax.broadcasted_iota(jnp.int32, (ntok, ntok), 0)
        col = lax.broadcasted_iota(jnp.int32, (ntok, ntok), 1)
        rank = dot(named, jnp.where(row < col, 1.0, 0.0).astype(BF16))
        slot = rank + (place(e_iota) * cap).astype(F32)
        return [jnp.sum(jnp.where(c, slot, 0.0), axis=0, keepdims=True) for c in chosen]

    wait_all(first_loads)
    lane_slots = slots_by_lane()

    sums = {0: (0, 2), 1: (1, 3), 4: (4,), 5: (5,), 6: (6,), 7: (7,)}
    units = sums
    unit_of = {u: u for u in sums}

    def slots_of(unit):
        first, count = rows_of(unit)
        return (lax.broadcasted_iota(jnp.int32, (count, ntok), 0) + first).astype(F32)

    def hits(unit):
        at = slots_of(unit)
        hit = (at == lane_slots[0]) | (at == lane_slots[1])
        return jnp.where(hit, 1.0, 0.0).astype(BF16)

    for unit in ((0, 2), (1, 3), (4, 6), (5, 7)):
        sent[span_of(unit)] = dot(hits(unit), x[...]).astype(BF16)
    rows[block(ep), mine] = sent[block(ep)]

    with scope("barrier"):
        pl.semaphore_wait(barrier, n_ep + 1)

    def remote(src, dst, sems, i, device, there=None):
        return pltpu.make_async_remote_copy(
            src_ref=src,
            dst_ref=dst,
            send_sem=sems.at[0, i],
            recv_sem=sems.at[1, i if there is None else there],
            device_id=device,
            device_id_type=MESH,
        )

    started = []

    def send(copy):
        copy.start()
        started.append(copy)

    halo_copies = [
        remote(ref.at[pl.ds(length - 16, 16)], halo.at[i], halo_sem, i, (next_ep, tp))
        for i, ref in enumerate((cgate, inputs))
    ]
    for copy in mix_loads[:2]:
        copy.wait()
    x_copy = remote(x, x_far, cross_sem, 0, (ep, far))
    for copy in halo_copies:
        send(copy)
    send(x_copy)

    def go_copy(j):
        to = flip(ep, j)
        return remote(
            sent.at[block(to)], rows.at[block(ep), mine], go_sem, j, (to, tp), seen_as(j)
        )

    def landed(dest, sems, j):
        block_of = dest.at[block(ep)] if dest is not rows else rows.at[block(ep), mine]
        remote(block_of, block_of, sems, j, (member(j), tp)).wait_recv()

    def go_far_copy(j):
        to = flip(ep, j)
        return remote(sent_far.at[block(to)], rows.at[block(ep), theirs], go_far_sem, j, (to, tp))

    go = {j: go_copy(j) for j in range(1, n_ep)}
    go_far = {j: go_far_copy(j) for j in range(1, n_ep // 2)}

    def depart(r):
        for j in run_of(r):
            if j:
                send(go[j])

    def pick_far():
        x_copy.wait_recv()
        for unit in ((0, 2), (1, 3)):
            sent_far[span_of(unit)] = dot(hits(unit), x_far[...]).astype(BF16)
        rows[block(ep), theirs] = sent_far[block(ep)]

    def depart_far(r):
        for j in run_of(r):
            if j:
                send(go_far[j])

    def hop(j, columns, sems, device):
        at = (block(member(j)), columns)
        return remote(rows.at[at], rows.at[at], sems, j, (ep, device))

    to_far = {j: hop(j, mine, far_sem, far) for j in range(n_ep // 2, n_ep)}
    to_near = [hop(j, mine, near_sem, near) for j in range(n_ep)]
    on_near = [hop(j, theirs, near2_sem, near) for j in range(n_ep)]

    def arrive(r):
        for j in run_of(r):
            if j:
                landed(rows, go_sem, j)
            if r >= 4:
                send(to_far[j])
            send(to_near[j])

    def arrive_far(r):
        for j in run_of(r):
            if j:
                go_far[j].wait_recv()
            send(on_near[j])

    def relay(r):
        for j in run_of(r):
            to_far[j].wait_recv()
            send(on_near[j])

    order = (cross, near, far, tp)

    part_copies = {}
    part_far_copies = {}

    def compute(u):
        unit = units[u]
        for r in unit:
            for j in run_of(r):
                to_near[j].wait_recv()
                on_near[j].wait_recv()
        span = span_of(unit)
        count = rows_of(unit)[1]
        wide = rows[span, :].astype(F32)
        scale = lax.rsqrt(jnp.sum(wide * wide, axis=1, keepdims=True) / d_all + 1e-06)
        normed[:count, :] = (wide * scale * gain[...]).astype(BF16)

        def tile(i, carry):
            columns = pl.ds(pl.multiple_of(i * 256, 256), 256)
            both = dot(normed[:count, :], wgu[:, columns])
            gate, upper = both[:, :128], both[:, 128:]
            act = gate / (1.0 + jnp.exp(-gate)) * upper
            hidden[:count, pl.ds(pl.multiple_of(i * 128, 128), 128)] = act.astype(BF16)
            return carry

        lax.fori_loop(0, tiles, tile, 0, unroll=True)

    def compute_down(u):
        span = span_of(units[u])
        count = rows_of(units[u])[1]
        for k, p in enumerate(order):
            columns = pl.ds(pl.multiple_of(p * d, 128), d)
            part[k, span] = dot(hidden[:count, :], wd[:, columns]).astype(BF16)
            if k < 2:
                part_copies[u, k] = remote(
                    part.at[k, span], part_in.at[k, span], part_sem, 2 * u + k, (ep, near)
                )
                send(part_copies[u, k])

    def part_wait(u, k):
        copy = part_copies.pop((unit_of[u], k), None)
        if copy is not None:
            copy.wait_recv()

    def send_back(u, source, dest, sems):
        for r in sums[u]:
            for j in run_of(r):
                if j == 0:
                    dest[block(ep)] = source[block(ep)]
                else:
                    to = member(j)
                    send(
                        remote(
                            source.at[block(to)],
                            dest.at[block(ep)],
                            sems,
                            j,
                            (to, tp),
                            seen_as(j),
                        )
                    )

    def add_near(u):
        span = span_of(sums[u])
        part_wait(u, 0)
        part_sum[span] = (part[2, span].astype(F32) + part_in[0, span].astype(F32)).astype(BF16)
        if u >= 4:
            part_far_copies[u] = remote(
                part_sum.at[span], part_far.at[span], part_far_sem, u, (ep, far)
            )
            send(part_far_copies[u])
        else:
            send_back(u, part_sum, back_far, back_far_sem)

    def add_own(u):
        span = span_of(sums[u])
        part_wait(u, 1)
        final[span] = (part[3, span].astype(F32) + part_in[1, span].astype(F32)).astype(BF16)
        send_back(u, final, back, back_sem)

    def add_far(u):
        span = span_of(sums[u])
        part_wait(u, 1)
        near_sum = part[3, span].astype(F32) + part_in[1, span].astype(F32)
        part_far_copies[u].wait_recv()
        final[span] = (near_sum + part_far[span].astype(F32)).astype(BF16)
        send_back(u, final, back, back_sem)

    total_copy = remote(total_out, total_in, cross_sem, 1, (ep, far))
    begun = set()

    def add_rows(into, span, got):
        now = sum(
            lax.dot_general(
                table[span], got[span], (((0,), (0,)), ((), ())), preferred_element_type=F32
            )
            for table in (at_high, at_low)
        )
        if id(into) in begun:
            into[...] += now
        else:
            into[...] = now
        begun.add(id(into))

    def collect(u):
        span = span_of(sums[u])
        for r in sums[u]:
            for j in run_of(r):
                if j:
                    landed(back, back_sem, j)
        add_rows(total, span, back)

    def collect_far(u):
        span = span_of(sums[u])
        for r in sums[u]:
            for j in run_of(r):
                if j:
                    landed(back_far, back_far_sem, j)
        add_rows(total_far, span, back_far)

    def swap_totals():
        total_out[...] = total_far[...].astype(BF16)
        send(total_copy)

    def finish():
        total_copy.wait_recv()
        routed[...] = (total[...] + total_in[...].astype(F32)).astype(BF16)
        for copy in started:
            copy.wait_send()

    part_rows = length // n_tp

    def part_of(p):
        return pl.ds(pl.multiple_of(p * part_rows, 16), part_rows)

    share_copies = []

    def gate_rows(first, count):
        conv = jnp.zeros((count, chans), F32)
        for j in range(reach + 1):
            start = 16 - reach + j + first
            conv = conv + taps[j : j + 1, :] * prod[start : start + count, :]
        return (bgate[first : first + count, :].astype(F32) * conv).astype(BF16)

    def mix():
        wait_all(mix_loads[2:])
        prod[0:16, :] = jnp.zeros((16, chans), F32)
        prod[16:, :] = cgate[...].astype(F32) * inputs[...].astype(F32)
        gated[...] = gate_rows(0, length)

        def tile(i, carry):
            columns = pl.ds(pl.multiple_of(i * 256, 256), 256)
            share[:, columns] = dot(gated[...], wo[:, columns]).astype(BF16)
            return carry

        lax.fori_loop(0, d_all // 256, tile, 0, unroll=True)

    def mix_first():
        for copy in halo_copies:
            copy.wait_recv()
        before = halo[0].astype(F32) * halo[1].astype(F32)
        prod[0:16, :] = jnp.where(ep > 0, before, 0.0)
        share[0:16, :] = dot(gate_rows(0, 16), wo[...]).astype(BF16)
        for k in range(2):
            share_copies.append(
                remote(share.at[part_of(order[k])], share_in.at[k], share_sem, k, (ep, near))
            )
            send(share_copies[k])

    def mix_near(q):
        if q == 0:
            share_copies[0].wait_recv()
        columns = pl.ds(q * d, d)
        share_sum[:, columns] = (
            share[part_of(far), columns].astype(F32) + share_in[0, :, columns].astype(F32)
        ).astype(BF16)
        share_copies.append(
            remote(
                share_sum.at[:, columns], share_far.at[:, columns], share_sem, 2 + q, (ep, far)
            )
        )
        send(share_copies[2 + q])

    def mix_far():
        share_copies[1].wait_recv()
        near_sum = share[part_of(tp), :].astype(F32) + share_in[1].astype(F32)
        for q in range(4):
            share_copies[2 + q].wait_recv()
        mixed[...] = (near_sum + share_far[...].astype(F32)).astype(BF16)

    def tables():
        wait_all(late_loads)
        for unit in units.values():
            at = slots_of(unit)
            value = jnp.where(at == lane_slots[0], weight_t[0:1, :], 0.0) + jnp.where(
                at == lane_slots[1], weight_t[1:2, :], 0.0
            )
            span = span_of(unit)
            at_high[span], at_low[span] = split_terms(value)

    tiles = ff // 128
    loads = []

    def load_weights():
        for i in range(tiles):
            columns = pl.ds(i * 128, 128)
            for source, sem, at in ((w_gate, gate_sem, 0), (w_up, up_sem, 128)):
                loads.append(
                    pltpu.make_async_copy(
                        source.at[0, :, columns], wgu.at[:, pl.ds(i * 256 + at, 128)], sem.at[i]
                    )
                )
        loads.append(pltpu.make_async_copy(w_down.at[0], wd, plain_sem.at[0]))
        for copy in loads:
            copy.start()

    def load_wait():
        wait_all(loads)

    steps = {
        "D": depart,
        "P": pick_far,
        "G": depart_far,
        "A": arrive,
        "B": arrive_far,
        "R": relay,
        "C": compute,
        "O": compute_down,
        "N": add_near,
        "F": add_far,
        "H": add_own,
        "K": collect,
        "M": collect_far,
        "W": swap_totals,
        "X": mix,
        "Q": mix_first,
        "Y": mix_near,
        "Z": mix_far,
        "T": tables,
        "S": load_weights,
        "L": load_wait,
        "E": finish,
    }
    for step in PLAN:
        with scope(step):
            steps[step[0]](*(int(c) for c in step[1:]))


def publish(mixed, routed, mixed_out, routed_out, sems):
    copies = [
        pltpu.make_async_copy(mixed, mixed_out, sems.at[0]),
        pltpu.make_async_copy(routed, routed_out, sems.at[1]),
    ]
    for copy in copies:
        copy.start()
    for copy in copies:
        copy.wait()


def body(
    mix_bgate,
    mix_cgate,
    mix_input,
    conv_taps,
    mix_out_w,
    moe_x,
    moe_gain,
    routes,
    route_w,
    w_gate,
    w_up,
    w_down,
):
    ntok, d = moe_x.shape
    length, chans = mix_input.shape
    n_ep = lax.axis_size("ep")
    n_tp = lax.axis_size("tp")
    assert w_gate.shape[0] == 1 and n_tp == 4 and routes.shape[1] == 2
    assert n_ep & (n_ep - 1) == 0
    cap = sizes_of(ntok, routes.shape[1], n_ep)
    assert n_ep % 8 == 0
    wide_rows = n_ep // 4 * cap
    d_all = n_tp * d
    ff = w_down.shape[1]
    slots = n_ep * cap
    part_rows = length // n_tp
    vmem = pl.BlockSpec(memory_space=pltpu.VMEM)
    anywhere = pl.BlockSpec(memory_space=pl.ANY)
    dma = pltpu.SemaphoreType.DMA
    call = pl.pallas_call(
        functools.partial(kernel, n_ep, n_tp, cap),
        out_shape=(
            pltpu.VMEM((part_rows, d_all), BF16),
            pltpu.VMEM((ntok, d), BF16),
        ),
        in_specs=[anywhere] * 12,
        out_specs=(vmem, vmem),
        scratch_shapes=[
            pltpu.VMEM((ntok, d), BF16),
            pltpu.VMEM((2, ntok), jnp.int32),
            pltpu.VMEM((length, chans), BF16),
            pltpu.VMEM((length, chans), BF16),
            pltpu.VMEM((length, chans), BF16),
            pltpu.VMEM(conv_taps.shape, F32),
            pltpu.VMEM((2, ntok), F32),
            pltpu.VMEM((1, d_all), F32),
            pltpu.VMEM((d_all, 2 * ff), BF16),
            pltpu.VMEM((ff, d_all), BF16),
            pltpu.VMEM((chans, d_all), BF16),
            pltpu.VMEM((2, 16, chans), BF16),
            pltpu.VMEM((16 + length, chans), F32),
            pltpu.VMEM((length, chans), BF16),
            pltpu.VMEM((length, d_all), BF16),
            pltpu.VMEM((2, part_rows, d_all), BF16),
            pltpu.VMEM((part_rows, d_all), BF16),
            pltpu.VMEM((part_rows, d_all), BF16),
            pltpu.VMEM((ntok, d), BF16),
            pltpu.VMEM((slots, d), BF16),
            pltpu.VMEM((slots, d), BF16),
            pltpu.VMEM((slots, d_all), BF16),
            pltpu.VMEM((wide_rows, d_all), BF16),
            pltpu.VMEM((wide_rows, ff), BF16),
            pltpu.VMEM((4, slots, d), BF16),
            pltpu.VMEM((2, slots, d), BF16),
            pltpu.VMEM((slots, d), BF16),
            pltpu.VMEM((slots, d), BF16),
            pltpu.VMEM((slots, d), BF16),
            pltpu.VMEM((slots, d), BF16),
            pltpu.VMEM((slots, d), BF16),
            pltpu.VMEM((slots, ntok), BF16),
            pltpu.VMEM((slots, ntok), BF16),
            pltpu.VMEM((ntok, d), F32),
            pltpu.VMEM((ntok, d), F32),
            pltpu.VMEM((ntok, d), BF16),
            pltpu.VMEM((ntok, d), BF16),
            dma((9,)),
            dma((ff // 128,)),
            dma((ff // 128,)),
            dma((1,)),
            dma((2, 2)),
            dma((2, 6)),
            dma((2, 2)),
            dma((2, n_ep)),
            dma((2, n_ep)),
            dma((2, n_ep)),
            dma((2, n_ep)),
            dma((2, n_ep)),
            dma((2, 16)),
            dma((2, 8)),
            dma((2, n_ep)),
            dma((2, n_ep)),
        ],
        compiler_params=pltpu.CompilerParams(
            collective_id=0, has_side_effects=True, vmem_limit_bytes=56 << 20
        ),
        name="step",
    )
    results = call(
        mix_bgate,
        mix_cgate,
        mix_input,
        conv_taps,
        mix_out_w,
        moe_x,
        moe_gain.reshape(1, d_all),
        routes.T,
        route_w.T,
        w_gate,
        w_up,
        w_down,
    )
    return pl.pallas_call(
        publish,
        out_shape=(
            jax.ShapeDtypeStruct((part_rows, d_all), BF16),
            jax.ShapeDtypeStruct((ntok, d), BF16),
        ),
        in_specs=[vmem, vmem],
        out_specs=(anywhere, anywhere),
        scratch_shapes=[dma((2,))],
        compiler_params=pltpu.CompilerParams(vmem_limit_bytes=1 << 20),
        name="publish",
    )(*results)


def solution(mesh):
    in_specs = (
        P("ep", "tp"),
        P("ep", "tp"),
        P("ep", "tp"),
        P(None, "tp"),
        P("tp", None),
        P("ep", "tp"),
        P(),
        P("ep", None),
        P("ep", None),
        P("ep", None, "tp"),
        P("ep", None, "tp"),
        P("ep", "tp", None),
    )
    out_specs = (P(("ep", "tp"), None), P("ep", "tp"))
    return jax.shard_map(body, mesh=mesh, in_specs=in_specs, out_specs=out_specs, check_vma=False)
```

```python
import functools

import jax
import jax.numpy as jnp
from jax import lax
from jax.experimental import pallas as pl
from jax.experimental.pallas import tpu as pltpu
from jax.sharding import PartitionSpec as P

BF16 = jnp.bfloat16
F32 = jnp.float32
MESH = pl.DeviceIdType.MESH
scope = jax.named_scope

PLAN = (
    "D6", "D4", "I", "D1", "D2", "D3", "A0", "S", "X", "T", "A1", "Q", "Y0", "A4", "P", "G2",
    "G1", "D7", "G3", "D5", "B0", "A2", "R4", "A6", "Y1", "L", "C4", "A3", "B2", "O4", "R6",
    "C0", "N4", "O0", "A5", "B1", "B3", "C6", "A7", "O6", "F4", "N6", "N0", "C1", "R5", "Y2",
    "O1", "Y3", "N1", "R7", "C5", "F6", "O5", "H0", "N5", "C7", "H1", "O7", "M0", "N7", "F5",
    "M1", "W", "F7", "Z", "K4", "K0", "K6", "K1", "K5", "K7", "E",
)


def flip(index, bits):
    bit = 1
    while bit <= bits:
        if bits & bit:
            index = index + bit - 2 * bit * ((index // bit) % 2)
        bit *= 2
    return index


def split_terms(value):
    high = value.astype(BF16)
    return high, (value - high.astype(F32)).astype(BF16)


def dot(a, b):
    return jnp.dot(a, b, preferred_element_type=F32)


def sizes_of(ntok, top, experts):
    cap = 4 * ((3 * ntok * top + 8 * experts - 1) // (8 * experts))
    return -(-cap // 16) * 16


def kernel(
    n_ep,
    n_tp,
    cap,
    bgate_in,
    cgate_in,
    inputs_in,
    taps_in,
    out_w,
    x_in,
    gain_in,
    routes_in,
    weight_in,
    w_gate,
    w_up,
    w_down,
    mixed,
    routed,
    x,
    routes_t,
    inputs,
    cgate,
    bgate,
    taps,
    weight_t,
    gain,
    wgu,
    wd,
    wo,
    halo,
    prod,
    gated,
    share,
    share_in,
    share_sum,
    share_far,
    x_far,
    sent,
    sent_far,
    rows,
    normed,
    hidden,
    part,
    part_in,
    part_sum,
    part_far,
    final,
    back,
    back_far,
    at_high,
    at_low,
    total,
    total_far,
    total_out,
    total_in,
    in_sem,
    gate_sem,
    up_sem,
    plain_sem,
    halo_sem,
    share_sem,
    cross_sem,
    go_sem,
    go_far_sem,
    far_sem,
    near_sem,
    near2_sem,
    part_sem,
    part_far_sem,
    back_sem,
    back_far_sem,
):
    ep = lax.axis_index("ep")
    tp = lax.axis_index("tp")
    ntok, d = x_in.shape
    length, chans = cgate_in.shape
    reach = taps_in.shape[0] - 1
    d_all = n_tp * d
    ff = w_down.shape[1]
    run_length = n_ep // 8
    near = flip(tp, 1)
    far = flip(tp, 2)
    cross = flip(tp, 3)
    mine = pl.ds(pl.multiple_of(tp * d, 128), d)
    theirs = pl.ds(pl.multiple_of(far * d, 128), d)
    next_ep = (ep + 1) % n_ep

    barrier = pltpu.get_barrier_semaphore()
    for j in range(1, n_ep):
        pl.semaphore_signal(barrier, inc=1, device_id=(flip(ep, j), tp), device_id_type=MESH)
    for t in (near, far):
        pl.semaphore_signal(barrier, inc=1, device_id=(ep, t), device_id_type=MESH)

    def load(i, source, dest):
        copy = pltpu.make_async_copy(source, dest, in_sem.at[i])
        copy.start()
        return copy

    first_loads = [load(0, routes_in, routes_t), load(1, x_in, x)]
    mix_loads = [
        load(2, inputs_in, inputs),
        load(3, cgate_in, cgate),
        load(4, bgate_in, bgate),
        load(5, taps_in, taps),
        load(6, out_w, wo),
    ]
    late_loads = [load(7, weight_in, weight_t), load(8, gain_in, gain)]

    def wait_all(copies):
        for copy in copies:
            copy.wait()
        copies.clear()

    def run_of(r):
        return range(r * run_length, (r + 1) * run_length)

    def place(i):
        low, run, high = i % run_length, i // run_length % 4, i // run_length // 4
        return (4 * high + 2 * (run % 2) + run // 2) * run_length + low

    def block(i):
        return pl.ds(pl.multiple_of(place(i) * cap, 16), cap)

    half = ep // (4 * run_length) % 2
    step = ep // (2 * run_length) % 2
    inner = half + step - 2 * half * step

    def member(j):
        to = flip(ep, j)
        if j < 4 * run_length:
            return to
        wanted = half if j // (2 * run_length) % 2 else 1 - half
        return to + 2 * run_length * (wanted - to // (2 * run_length) % 2)

    def seen_as(j):
        if j < 4 * run_length:
            return j
        run, low = j // run_length, j % run_length
        return (4 + 2 * inner + run % 2) * run_length + low

    def rows_of(unit):
        count = len(unit) * run_length
        first = place(member(unit[0] * run_length)) // count * count * cap
        return first, count * cap

    def span_of(unit):
        first, count = rows_of(unit)
        return pl.ds(pl.multiple_of(first, 16), count)

    def slots_by_lane():
        e_iota = lax.broadcasted_iota(jnp.int32, (n_ep, ntok), 0)
        chosen = [routes_t[k : k + 1, :] == e_iota for k in range(2)]
        named = jnp.where(chosen[0] | chosen[1], 1.0, 0.0).astype(BF16)
        row = lax.broadcasted_iota(jnp.int32, (ntok, ntok), 0)
        col = lax.broadcasted_iota(jnp.int32, (ntok, ntok), 1)
        rank = dot(named, jnp.where(row < col, 1.0, 0.0).astype(BF16))
        slot = rank + (place(e_iota) * cap).astype(F32)
        return [jnp.sum(jnp.where(c, slot, 0.0), axis=0, keepdims=True) for c in chosen]

    wait_all(first_loads)
    lane_slots = slots_by_lane()

    sums = {0: (0, 2), 1: (1, 3), 4: (4,), 5: (5,), 6: (6,), 7: (7,)}
    units = sums
    unit_of = {u: u for u in sums}

    def slots_of(unit):
        first, count = rows_of(unit)
        return (lax.broadcasted_iota(jnp.int32, (count, ntok), 0) + first).astype(F32)

    def hits(unit):
        at = slots_of(unit)
        hit = (at == lane_slots[0]) | (at == lane_slots[1])
        return jnp.where(hit, 1.0, 0.0).astype(BF16)

    def pick(unit):
        sent[span_of(unit)] = dot(hits(unit), x[...]).astype(BF16)

    pick((4, 6))
    with scope("barrier"):
        pl.semaphore_wait(barrier, n_ep + 1)

    def remote(src, dst, sems, i, device, there=None):
        return pltpu.make_async_remote_copy(
            src_ref=src,
            dst_ref=dst,
            send_sem=sems.at[0, i],
            recv_sem=sems.at[1, i if there is None else there],
            device_id=device,
            device_id_type=MESH,
        )

    started = []

    def send(copy):
        copy.start()
        started.append(copy)

    halo_copies = [
        remote(ref.at[pl.ds(length - 16, 16)], halo.at[i], halo_sem, i, (next_ep, tp))
        for i, ref in enumerate((cgate, inputs))
    ]
    for copy in mix_loads[:2]:
        copy.wait()
    x_copy = remote(x, x_far, cross_sem, 0, (ep, far))
    for copy in halo_copies:
        send(copy)
    send(x_copy)

    def go_copy(j):
        to = flip(ep, j)
        return remote(
            sent.at[block(to)], rows.at[block(ep), mine], go_sem, j, (to, tp), seen_as(j)
        )

    def landed(dest, sems, j):
        block_of = dest.at[block(ep)] if dest is not rows else rows.at[block(ep), mine]
        remote(block_of, block_of, sems, j, (member(j), tp)).wait_recv()

    def go_far_copy(j):
        to = flip(ep, j)
        return remote(sent_far.at[block(to)], rows.at[block(ep), theirs], go_far_sem, j, (to, tp))

    go = {j: go_copy(j) for j in range(1, n_ep)}
    go_far = {j: go_far_copy(j) for j in range(1, n_ep // 2)}

    def pick_rest():
        for unit in ((0, 2), (1, 3), (5, 7)):
            pick(unit)
        rows[block(ep), mine] = sent[block(ep)]

    def depart(r):
        for j in run_of(r):
            if j:
                send(go[j])

    def pick_far():
        x_copy.wait_recv()
        for unit in ((0, 2), (1, 3)):
            sent_far[span_of(unit)] = dot(hits(unit), x_far[...]).astype(BF16)
        rows[block(ep), theirs] = sent_far[block(ep)]

    def depart_far(r):
        for j in run_of(r):
            if j:
                send(go_far[j])

    def hop(j, columns, sems, device):
        at = (block(member(j)), columns)
        return remote(rows.at[at], rows.at[at], sems, j, (ep, device))

    to_far = {j: hop(j, mine, far_sem, far) for j in range(n_ep // 2, n_ep)}
    to_near = [hop(j, mine, near_sem, near) for j in range(n_ep)]
    on_near = [hop(j, theirs, near2_sem, near) for j in range(n_ep)]

    def arrive(r):
        for j in run_of(r):
            if j:
                landed(rows, go_sem, j)
            if r >= 4:
                send(to_far[j])
            send(to_near[j])

    def arrive_far(r):
        for j in run_of(r):
            if j:
                go_far[j].wait_recv()
            send(on_near[j])

    def relay(r):
        for j in run_of(r):
            to_far[j].wait_recv()
            send(on_near[j])

    order = (cross, near, far, tp)

    part_copies = {}
    part_far_copies = {}

    def compute(u):
        unit = units[u]
        for r in unit:
            for j in run_of(r):
                to_near[j].wait_recv()
                on_near[j].wait_recv()
        span = span_of(unit)
        count = rows_of(unit)[1]
        wide = rows[span, :].astype(F32)
        scale = lax.rsqrt(jnp.sum(wide * wide, axis=1, keepdims=True) / d_all + 1e-06)
        normed[:count, :] = (wide * scale * gain[...]).astype(BF16)

        def tile(i, carry):
            columns = pl.ds(pl.multiple_of(i * 256, 256), 256)
            both = dot(normed[:count, :], wgu[:, columns])
            gate, upper = both[:, :128], both[:, 128:]
            act = gate / (1.0 + jnp.exp(-gate)) * upper
            hidden[:count, pl.ds(pl.multiple_of(i * 128, 128), 128)] = act.astype(BF16)
            return carry

        lax.fori_loop(0, tiles, tile, 0, unroll=True)

    def compute_down(u):
        span = span_of(units[u])
        count = rows_of(units[u])[1]
        for k, p in enumerate(order):
            columns = pl.ds(pl.multiple_of(p * d, 128), d)
            part[k, span] = dot(hidden[:count, :], wd[:, columns]).astype(BF16)
            if k < 2:
                part_copies[u, k] = remote(
                    part.at[k, span], part_in.at[k, span], part_sem, 2 * u + k, (ep, near)
                )
                send(part_copies[u, k])

    def part_wait(u, k):
        copy = part_copies.pop((unit_of[u], k), None)
        if copy is not None:
            copy.wait_recv()

    def send_back(u, source, dest, sems):
        for r in sums[u]:
            for j in run_of(r):
                if j == 0:
                    dest[block(ep)] = source[block(ep)]
                else:
                    to = member(j)
                    send(
                        remote(
                            source.at[block(to)],
                            dest.at[block(ep)],
                            sems,
                            j,
                            (to, tp),
                            seen_as(j),
                        )
                    )

    def add_near(u):
        span = span_of(sums[u])
        part_wait(u, 0)
        part_sum[span] = (part[2, span].astype(F32) + part_in[0, span].astype(F32)).astype(BF16)
        if u >= 4:
            part_far_copies[u] = remote(
                part_sum.at[span], part_far.at[span], part_far_sem, u, (ep, far)
            )
            send(part_far_copies[u])
        else:
            send_back(u, part_sum, back_far, back_far_sem)

    def add_own(u):
        span = span_of(sums[u])
        part_wait(u, 1)
        final[span] = (part[3, span].astype(F32) + part_in[1, span].astype(F32)).astype(BF16)
        send_back(u, final, back, back_sem)

    def add_far(u):
        span = span_of(sums[u])
        part_wait(u, 1)
        near_sum = part[3, span].astype(F32) + part_in[1, span].astype(F32)
        part_far_copies[u].wait_recv()
        final[span] = (near_sum + part_far[span].astype(F32)).astype(BF16)
        send_back(u, final, back, back_sem)

    total_copy = remote(total_out, total_in, cross_sem, 1, (ep, far))
    begun = set()

    def add_rows(into, span, got):
        now = sum(
            lax.dot_general(
                table[span], got[span], (((0,), (0,)), ((), ())), preferred_element_type=F32
            )
            for table in (at_high, at_low)
        )
        if id(into) in begun:
            into[...] += now
        else:
            into[...] = now
        begun.add(id(into))

    def collect(u):
        span = span_of(sums[u])
        for r in sums[u]:
            for j in run_of(r):
                if j:
                    landed(back, back_sem, j)
        add_rows(total, span, back)

    def collect_far(u):
        span = span_of(sums[u])
        for r in sums[u]:
            for j in run_of(r):
                if j:
                    landed(back_far, back_far_sem, j)
        add_rows(total_far, span, back_far)

    def swap_totals():
        total_out[...] = total_far[...].astype(BF16)
        send(total_copy)

    def finish():
        total_copy.wait_recv()
        routed[...] = (total[...] + total_in[...].astype(F32)).astype(BF16)
        for copy in started:
            copy.wait_send()

    part_rows = length // n_tp

    def part_of(p):
        return pl.ds(pl.multiple_of(p * part_rows, 16), part_rows)

    share_copies = []

    def gate_rows(first, count):
        conv = jnp.zeros((count, chans), F32)
        for j in range(reach + 1):
            start = 16 - reach + j + first
            conv = conv + taps[j : j + 1, :] * prod[start : start + count, :]
        return (bgate[first : first + count, :].astype(F32) * conv).astype(BF16)

    def mix():
        wait_all(mix_loads[2:])
        prod[0:16, :] = jnp.zeros((16, chans), F32)
        prod[16:, :] = cgate[...].astype(F32) * inputs[...].astype(F32)
        gated[...] = gate_rows(0, length)

        def tile(i, carry):
            columns = pl.ds(pl.multiple_of(i * 256, 256), 256)
            share[:, columns] = dot(gated[...], wo[:, columns]).astype(BF16)
            return carry

        lax.fori_loop(0, d_all // 256, tile, 0, unroll=True)

    def mix_first():
        for copy in halo_copies:
            copy.wait_recv()
        before = halo[0].astype(F32) * halo[1].astype(F32)
        prod[0:16, :] = jnp.where(ep > 0, before, 0.0)
        share[0:16, :] = dot(gate_rows(0, 16), wo[...]).astype(BF16)
        for k in range(2):
            share_copies.append(
                remote(share.at[part_of(order[k])], share_in.at[k], share_sem, k, (ep, near))
            )
            send(share_copies[k])

    def mix_near(q):
        if q == 0:
            share_copies[0].wait_recv()
        columns = pl.ds(q * d, d)
        share_sum[:, columns] = (
            share[part_of(far), columns].astype(F32) + share_in[0, :, columns].astype(F32)
        ).astype(BF16)
        share_copies.append(
            remote(
                share_sum.at[:, columns], share_far.at[:, columns], share_sem, 2 + q, (ep, far)
            )
        )
        send(share_copies[2 + q])

    def mix_far():
        share_copies[1].wait_recv()
        near_sum = share[part_of(tp), :].astype(F32) + share_in[1].astype(F32)
        for q in range(4):
            share_copies[2 + q].wait_recv()
        mixed[...] = (near_sum + share_far[...].astype(F32)).astype(BF16)

    def tables():
        wait_all(late_loads)
        for unit in units.values():
            at = slots_of(unit)
            value = jnp.where(at == lane_slots[0], weight_t[0:1, :], 0.0) + jnp.where(
                at == lane_slots[1], weight_t[1:2, :], 0.0
            )
            span = span_of(unit)
            at_high[span], at_low[span] = split_terms(value)

    tiles = ff // 128
    loads = []

    def load_weights():
        for i in range(tiles):
            columns = pl.ds(i * 128, 128)
            for source, sem, at in ((w_gate, gate_sem, 0), (w_up, up_sem, 128)):
                loads.append(
                    pltpu.make_async_copy(
                        source.at[0, :, columns], wgu.at[:, pl.ds(i * 256 + at, 128)], sem.at[i]
                    )
                )
        loads.append(pltpu.make_async_copy(w_down.at[0], wd, plain_sem.at[0]))
        for copy in loads:
            copy.start()

    def load_wait():
        wait_all(loads)

    steps = {
        "D": depart,
        "I": pick_rest,
        "P": pick_far,
        "G": depart_far,
        "A": arrive,
        "B": arrive_far,
        "R": relay,
        "C": compute,
        "O": compute_down,
        "N": add_near,
        "F": add_far,
        "H": add_own,
        "K": collect,
        "M": collect_far,
        "W": swap_totals,
        "X": mix,
        "Q": mix_first,
        "Y": mix_near,
        "Z": mix_far,
        "T": tables,
        "S": load_weights,
        "L": load_wait,
        "E": finish,
    }
    for step in PLAN:
        with scope(step):
            steps[step[0]](*(int(c) for c in step[1:]))


def publish(mixed, routed, mixed_out, routed_out, sems):
    copies = [
        pltpu.make_async_copy(mixed, mixed_out, sems.at[0]),
        pltpu.make_async_copy(routed, routed_out, sems.at[1]),
    ]
    for copy in copies:
        copy.start()
    for copy in copies:
        copy.wait()


def body(
    mix_bgate,
    mix_cgate,
    mix_input,
    conv_taps,
    mix_out_w,
    moe_x,
    moe_gain,
    routes,
    route_w,
    w_gate,
    w_up,
    w_down,
):
    ntok, d = moe_x.shape
    length, chans = mix_input.shape
    n_ep = lax.axis_size("ep")
    n_tp = lax.axis_size("tp")
    assert w_gate.shape[0] == 1 and n_tp == 4 and routes.shape[1] == 2
    assert n_ep & (n_ep - 1) == 0
    cap = sizes_of(ntok, routes.shape[1], n_ep)
    assert n_ep % 8 == 0
    wide_rows = n_ep // 4 * cap
    d_all = n_tp * d
    ff = w_down.shape[1]
    slots = n_ep * cap
    part_rows = length // n_tp
    vmem = pl.BlockSpec(memory_space=pltpu.VMEM)
    anywhere = pl.BlockSpec(memory_space=pl.ANY)
    dma = pltpu.SemaphoreType.DMA
    call = pl.pallas_call(
        functools.partial(kernel, n_ep, n_tp, cap),
        out_shape=(
            pltpu.VMEM((part_rows, d_all), BF16),
            pltpu.VMEM((ntok, d), BF16),
        ),
        in_specs=[anywhere] * 12,
        out_specs=(vmem, vmem),
        scratch_shapes=[
            pltpu.VMEM((ntok, d), BF16),
            pltpu.VMEM((2, ntok), jnp.int32),
            pltpu.VMEM((length, chans), BF16),
            pltpu.VMEM((length, chans), BF16),
            pltpu.VMEM((length, chans), BF16),
            pltpu.VMEM(conv_taps.shape, F32),
            pltpu.VMEM((2, ntok), F32),
            pltpu.VMEM((1, d_all), F32),
            pltpu.VMEM((d_all, 2 * ff), BF16),
            pltpu.VMEM((ff, d_all), BF16),
            pltpu.VMEM((chans, d_all), BF16),
            pltpu.VMEM((2, 16, chans), BF16),
            pltpu.VMEM((16 + length, chans), F32),
            pltpu.VMEM((length, chans), BF16),
            pltpu.VMEM((length, d_all), BF16),
            pltpu.VMEM((2, part_rows, d_all), BF16),
            pltpu.VMEM((part_rows, d_all), BF16),
            pltpu.VMEM((part_rows, d_all), BF16),
            pltpu.VMEM((ntok, d), BF16),
            pltpu.VMEM((slots, d), BF16),
            pltpu.VMEM((slots, d), BF16),
            pltpu.VMEM((slots, d_all), BF16),
            pltpu.VMEM((wide_rows, d_all), BF16),
            pltpu.VMEM((wide_rows, ff), BF16),
            pltpu.VMEM((4, slots, d), BF16),
            pltpu.VMEM((2, slots, d), BF16),
            pltpu.VMEM((slots, d), BF16),
            pltpu.VMEM((slots, d), BF16),
            pltpu.VMEM((slots, d), BF16),
            pltpu.VMEM((slots, d), BF16),
            pltpu.VMEM((slots, d), BF16),
            pltpu.VMEM((slots, ntok), BF16),
            pltpu.VMEM((slots, ntok), BF16),
            pltpu.VMEM((ntok, d), F32),
            pltpu.VMEM((ntok, d), F32),
            pltpu.VMEM((ntok, d), BF16),
            pltpu.VMEM((ntok, d), BF16),
            dma((9,)),
            dma((ff // 128,)),
            dma((ff // 128,)),
            dma((1,)),
            dma((2, 2)),
            dma((2, 6)),
            dma((2, 2)),
            dma((2, n_ep)),
            dma((2, n_ep)),
            dma((2, n_ep)),
            dma((2, n_ep)),
            dma((2, n_ep)),
            dma((2, 16)),
            dma((2, 8)),
            dma((2, n_ep)),
            dma((2, n_ep)),
        ],
        compiler_params=pltpu.CompilerParams(
            collective_id=0, has_side_effects=True, vmem_limit_bytes=56 << 20
        ),
        name="step",
    )
    results = call(
        mix_bgate,
        mix_cgate,
        mix_input,
        conv_taps,
        mix_out_w,
        moe_x,
        moe_gain.reshape(1, d_all),
        routes.T,
        route_w.T,
        w_gate,
        w_up,
        w_down,
    )
    return pl.pallas_call(
        publish,
        out_shape=(
            jax.ShapeDtypeStruct((part_rows, d_all), BF16),
            jax.ShapeDtypeStruct((ntok, d), BF16),
        ),
        in_specs=[vmem, vmem],
        out_specs=(anywhere, anywhere),
        scratch_shapes=[dma((2,))],
        compiler_params=pltpu.CompilerParams(vmem_limit_bytes=1 << 20),
        name="publish",
    )(*results)


def solution(mesh):
    in_specs = (
        P("ep", "tp"),
        P("ep", "tp"),
        P("ep", "tp"),
        P(None, "tp"),
        P("tp", None),
        P("ep", "tp"),
        P(),
        P("ep", None),
        P("ep", None),
        P("ep", None, "tp"),
        P("ep", None, "tp"),
        P("ep", "tp", None),
    )
    out_specs = (P(("ep", "tp"), None), P("ep", "tp"))
    return jax.shard_map(body, mesh=mesh, in_specs=in_specs, out_specs=out_specs, check_vma=False)
```
